32 devices in a mesh: rep: 2 (over x), fs: 8 (over z, y), tp: 2 (over core).
Axes of the slice: x: 2, y: 2, z: 4, core: 2. Of those that a mesh axis runs over, the one named last changes fastest.
Arguments:
- tokens: bfloat16 [10240, 2048], P(('rep', 'fs', 'tp')), may hold values from -6 to 6
- mix_gain: float32 [2048], replicated, may hold values from 0.1 to 1.9
- w_bgate: bfloat16 [2048, 2048], P('fs', 'tp'), may hold values from -0.125 to 0.125
- w_cgate: bfloat16 [2048, 2048], P('fs', 'tp'), may hold values from -0.125 to 0.125
- w_value: bfloat16 [2048, 2048], P('fs', 'tp'), may hold values from -0.125 to 0.125
- conv_taps: float32 [3, 2048], replicated, may hold values from -3 to 3
- w_mixout: bfloat16 [2048, 2048], P('tp', 'fs'), may hold values from -0.125 to 0.125
- mlp_gain: float32 [2048], replicated, may hold values from 0.1 to 1.9
- w_gate: bfloat16 [2048, 2816], P('fs', 'tp'), may hold values from -0.125 to 0.125
- w_up: bfloat16 [2048, 2816], P('fs', 'tp'), may hold values from -0.125 to 0.125
- w_down: bfloat16 [2816, 2048], P('tp', 'fs'), may hold values from -0.109375 to 0.109375
Outputs:
- block_out: bfloat16 [10240, 2048], P(('rep', 'fs', 'tp'))
The draws below stay inside these ranges and needn't reach their ends.
All inputs are finite; a program needn't handle non-finite values.
Results may differ from the reference program's by a relative error of at most 0.0085.
Values may be sent and summed in bfloat16 or wider, within the bound.
A program may use at most 128 MiB of HBM per device.

```python
import jax
import jax.numpy as jnp
from jax import lax

D = 2048
FF = 2816
LENGTH = 640
TOKENS = 10240
N_TP = 2


def block_scale(key, extent, split, least, top_value):
    level, own = 1.0, jax.random.fold_in(key, 6)
    for dim, blocks in split:
        steps = jnp.exp(jax.random.uniform(jax.random.fold_in(own, dim), (blocks,), jnp.float32, least / len(split), top_value / len(split)))
        level = level * jnp.repeat(steps, extent[dim] // blocks).reshape([-1 if axis == dim else 1 for axis in range(len(extent))])
    return level


def centred(own_key, extent, width, bound, cuts=(), dtype=jnp.bfloat16):
    drawn = jax.random.normal(own_key, extent, jnp.float32) * width
    if len(cuts) > 0:
        drawn = block_scale(own_key, extent, cuts, -0.22, 0.18) * drawn
    return jnp.clip(drawn, min=-bound, max=bound).astype(dtype)


def setup_inputs(seed: int = 0) -> dict:
    key_of = jax.random.split(jax.random.key(seed), 12)
    tokens = centred(key_of[0], (TOKENS, D), 1.0, 6.0, ((0, 32),))
    mix_gain = jnp.clip(1.0 + 0.18 * jax.random.normal(key_of[1], (D,), jnp.float32), 0.1, 1.9)
    w_bgate = centred(key_of[2], (D, D), D ** -0.5, 0.125, ((0, 8), (1, 2)))
    w_cgate = centred(key_of[3], (D, D), D ** -0.5, 0.125, ((0, 8), (1, 2)))
    w_value = centred(key_of[4], (D, D), D ** -0.5, 0.125, ((0, 8), (1, 2)))
    conv_taps = centred(key_of[5], (3, D), 0.6, 3.0, (), jnp.float32)
    w_mixout = centred(key_of[6], (D, D), D ** -0.5, 0.125, ((0, 2), (1, 8)))
    mlp_gain = jnp.clip(1.0 + 0.18 * jax.random.normal(key_of[7], (D,), jnp.float32), 0.1, 1.9)
    w_gate = centred(key_of[8], (D, FF), D ** -0.5, 0.125, ((0, 8), (1, 2)))
    w_up = centred(key_of[9], (D, FF), D ** -0.5, 0.125, ((0, 8), (1, 2)))
    w_down = centred(key_of[10], (FF, D), FF ** -0.5, 0.109375, ((0, 2), (1, 8)))
    return {"tokens": tokens, "mix_gain": mix_gain, "w_bgate": w_bgate, "w_cgate": w_cgate, "w_value": w_value, "conv_taps": conv_taps, "w_mixout": w_mixout, "mlp_gain": mlp_gain, "w_gate": w_gate, "w_up": w_up, "w_down": w_down}


def rms_scale(matrix, gain):
    values = matrix.astype(jnp.float32)
    factor = lax.rsqrt(lax.optimization_barrier(jnp.mean(values * values, axis=-1, keepdims=True)) + 1e-06)
    return values * factor * gain.astype(jnp.float32)

def causal_taps(mixed, filters):
    length = mixed.shape[-2]
    widths = [(0, 0)] * (mixed.ndim - 2) + [(2, 0), (0, 0)]
    padded = jnp.pad(mixed, widths)
    return filters[0] * padded[..., 0:length, :] + filters[1] * padded[..., 1:length + 1, :] + filters[2] * padded[..., 2:length + 2, :]

def split_sum(left, right):
    portion = left.shape[1] // N_TP
    running = jnp.zeros((left.shape[0], right.shape[1]), jnp.float32)
    for member in range(N_TP):
        partial_out = jnp.dot(left[:, member * portion:(member + 1) * portion], right[member * portion:(member + 1) * portion], preferred_element_type=jnp.float32)
        partial_out = lax.optimization_barrier(partial_out.astype(jnp.bfloat16))
        running = running + partial_out.astype(jnp.float32)
    return running

def reference(tokens, mix_gain, w_bgate, w_cgate, w_value, conv_taps, w_mixout, mlp_gain, w_gate, w_up, w_down):
    normed = rms_scale(tokens, mix_gain).astype(jnp.bfloat16)
    b_proj = jnp.dot(normed, w_bgate, preferred_element_type=jnp.float32).astype(jnp.bfloat16)
    c_proj = jnp.dot(normed, w_cgate, preferred_element_type=jnp.float32).astype(jnp.bfloat16)
    u_proj = jnp.dot(normed, w_value, preferred_element_type=jnp.float32).astype(jnp.bfloat16)
    mixed_in = c_proj.astype(jnp.float32) * u_proj.astype(jnp.float32)
    mixed_in = mixed_in.reshape(TOKENS // LENGTH, LENGTH, D)
    convolved = causal_taps(mixed_in, conv_taps).reshape(TOKENS, D)
    gated = (b_proj.astype(jnp.float32) * convolved).astype(jnp.bfloat16)
    residual = tokens.astype(jnp.float32) + split_sum(gated, w_mixout)
    normed_two = rms_scale(residual, mlp_gain).astype(jnp.bfloat16)
    gate = jnp.dot(normed_two, w_gate, preferred_element_type=jnp.float32)
    up_value = jnp.dot(normed_two, w_up, preferred_element_type=jnp.float32)
    hidden = (jax.nn.silu(gate) * up_value).astype(jnp.bfloat16)
    return (residual + 0.5 * split_sum(hidden, w_down)).astype(jnp.bfloat16)
```

```python
import jax
import jax.numpy as jnp
from jax import lax
from jax.sharding import PartitionSpec as P


def rms_scale(matrix, gain):
    values = matrix.astype(jnp.float32)
    factor = lax.rsqrt(jnp.mean(values * values, axis=-1, keepdims=True) + 1e-06)
    return values * factor * gain


def causal_taps(mixed, filters):
    length = mixed.shape[-2]
    padded = jnp.pad(mixed, [(2, 0), (0, 0)])
    return (
        filters[0] * padded[0:length]
        + filters[1] * padded[1 : length + 1]
        + filters[2] * padded[2 : length + 2]
    )


def swap(array, axis):
    return lax.ppermute(array, axis, [(0, 1), (1, 0)])


def half(array, axis, part):
    size = array.shape[axis] // 2
    return lax.dynamic_slice_in_dim(array, part * size, size, axis)


def build(n_fs):
    ring = [(i, (i + 2) % n_fs) for i in range(n_fs)]
    pair = [(i, i ^ 1) for i in range(n_fs)]
    steps = n_fs // 2

    def ring_first(block):
        blocks = []
        for step in range(steps):
            blocks += [block, lax.ppermute(block, "fs", pair)]
            if step < steps - 1:
                block = lax.ppermute(block, "fs", ring)
        return blocks

    def pair_first(block):
        mate = lax.ppermute(block, "fs", pair)
        blocks = []
        for step in range(steps):
            blocks += [block, mate]
            if step < steps - 1:
                block, mate = lax.ppermute(block, "fs", ring), lax.ppermute(mate, "fs", ring)
        return blocks

    def on_device(
        tokens, mix_gain, w_bgate, w_cgate, w_value, conv_taps, w_mixout, mlp_gain, w_gate, w_up, w_down
    ):
        rep, fs, tp = (lax.axis_index(name) for name in ("rep", "fs", "tp"))
        width = tokens.shape[1] // n_fs

        def arrival_order(array):
            order = [((fs ^ j) - 2 * s + n_fs) % n_fs for s in range(steps) for j in range(2)]
            return jnp.concatenate(
                [lax.dynamic_slice_in_dim(array, k * width, width, array.ndim - 1) for k in order],
                axis=-1,
            )

        def global_order(array):
            places = []
            for k in range(n_fs):
                j = (fs ^ k) & 1
                places.append((((fs ^ j) - k + n_fs) % n_fs) + j)
            return jnp.concatenate(
                [lax.dynamic_slice_in_dim(array, k * width, width, array.ndim - 1) for k in places],
                axis=-1,
            )

        def sequence(rows):
            other = swap(rows, "tp")
            return jnp.concatenate(
                [jnp.where(tp == 0, rows, other), jnp.where(tp == 0, other, rows)], axis=0
            )

        def both_sequences(rows):
            return sequence(rows), sequence(swap(rows, "rep"))

        def chip_sum(partial):
            other = swap(half(partial, 0, 1 - tp), "tp")
            return half(partial, 0, tp).astype(jnp.float32) + other.astype(jnp.float32)

        def project_out(mine, theirs, blocks, group):
            sums = []
            for start in range(0, len(blocks), group):
                weight = jnp.concatenate(blocks[start : start + group], axis=1)
                outs = [
                    jnp.dot(rows, weight, preferred_element_type=jnp.float32).astype(jnp.bfloat16)
                    for rows in (theirs, mine)
                ]
                away = swap(chip_sum(outs[0]).astype(jnp.bfloat16), "rep")
                sums.append(chip_sum(outs[1]) + away.astype(jnp.float32))
            return jnp.concatenate(sums, axis=1)

        w_in = jnp.concatenate([half(w, 1, rep) for w in (w_bgate, w_cgate, w_value)], axis=1)
        w_gu = jnp.concatenate([half(w, 1, rep) for w in (w_gate, w_up)], axis=1)
        in_blocks = ring_first(w_in)
        out_blocks = ring_first(half(w_mixout, 0, rep))
        gu_blocks = ring_first(w_gu)
        down_blocks = pair_first(half(w_down, 0, rep))

        channels = w_in.shape[1] // 3
        taps = lax.dynamic_slice_in_dim(conv_taps, (tp * 2 + rep) * channels, channels, 1)
        local = arrival_order(tokens)

        def mix(normed, weight):
            projected = jnp.dot(normed, weight, preferred_element_type=jnp.float32).astype(
                jnp.bfloat16
            )
            b_proj, c_proj, u_proj = (
                projected[:, k * channels : (k + 1) * channels].astype(jnp.float32)
                for k in range(3)
            )
            return (b_proj * causal_taps(c_proj * u_proj, taps)).astype(jnp.bfloat16)

        mine, theirs = both_sequences(
            rms_scale(local, arrival_order(mix_gain)).astype(jnp.bfloat16)
        )
        weight = jnp.concatenate(in_blocks, axis=0)
        mixed = project_out(mix(mine, weight), mix(theirs, weight), out_blocks, n_fs)
        residual = local.astype(jnp.float32) + mixed

        units = w_gu.shape[1] // 2

        def feed(normed, weight):
            both = jnp.dot(normed, weight, preferred_element_type=jnp.float32)
            return (jax.nn.silu(both[:, :units]) * both[:, units:]).astype(jnp.bfloat16)

        mine, theirs = both_sequences(
            rms_scale(residual, arrival_order(mlp_gain)).astype(jnp.bfloat16)
        )
        weight = jnp.concatenate(gu_blocks, axis=0)
        down = project_out(feed(mine, weight), feed(theirs, weight), down_blocks, 2)
        return global_order((residual + 0.5 * down).astype(jnp.bfloat16))

    return on_device


def solution(mesh):
    return jax.shard_map(
        build(mesh.shape["fs"]),
        mesh=mesh,
        in_specs=(
            P(("rep", "fs", "tp"), None),
            P(),
            P("fs", "tp"),
            P("fs", "tp"),
            P("fs", "tp"),
            P(),
            P("tp", "fs"),
            P(),
            P("fs", "tp"),
            P("fs", "tp"),
            P("tp", "fs"),
        ),
        out_specs=P(("rep", "fs", "tp"), None),
        check_vma=False,
    )
```

```python
import jax
import jax.numpy as jnp
from jax import lax
from jax.sharding import PartitionSpec as P


def rms_scale(matrix, gain):
    values = matrix.astype(jnp.float32)
    factor = lax.rsqrt(jnp.mean(values * values, axis=-1, keepdims=True) + 1e-06)
    return values * factor * gain


def causal_taps(mixed, filters):
    length = mixed.shape[-2]
    padded = jnp.pad(mixed, [(2, 0), (0, 0)])
    return (
        filters[0] * padded[0:length]
        + filters[1] * padded[1 : length + 1]
        + filters[2] * padded[2 : length + 2]
    )


def swap(array, axis):
    return lax.ppermute(array, axis, [(0, 1), (1, 0)])


def half(array, axis, part):
    size = array.shape[axis] // 2
    return lax.dynamic_slice_in_dim(array, part * size, size, axis)


def build(n_fs):
    ring = [(i, (i + 2) % n_fs) for i in range(n_fs)]
    pair = [(i, i ^ 1) for i in range(n_fs)]
    steps = n_fs // 2

    def ring_first(block):
        blocks = []
        for step in range(steps):
            blocks += [block, lax.ppermute(block, "fs", pair)]
            if step < steps - 1:
                block = lax.ppermute(block, "fs", ring)
        return blocks

    def pair_first(block):
        mate = lax.ppermute(block, "fs", pair)
        blocks = []
        for step in range(steps):
            blocks += [block, mate]
            if step < steps - 1:
                block = lax.ppermute(block, "fs", ring)
                mate = lax.ppermute(mate, "fs", ring)
        return blocks

    def on_device(
        tokens, mix_gain, w_bgate, w_cgate, w_value, conv_taps, w_mixout, mlp_gain, w_gate, w_up, w_down
    ):
        rep, fs, tp = (lax.axis_index(name) for name in ("rep", "fs", "tp"))
        width = tokens.shape[1] // n_fs

        def arrival_order(array):
            order = [((fs ^ j) - 2 * s + n_fs) % n_fs for s in range(steps) for j in range(2)]
            return jnp.concatenate(
                [lax.dynamic_slice_in_dim(array, k * width, width, array.ndim - 1) for k in order],
                axis=-1,
            )

        def global_order(array):
            places = []
            for k in range(n_fs):
                j = (fs ^ k) & 1
                places.append((((fs ^ j) - k + n_fs) % n_fs) + j)
            return jnp.concatenate(
                [lax.dynamic_slice_in_dim(array, k * width, width, array.ndim - 1) for k in places],
                axis=-1,
            )

        def sequence(rows):
            other = swap(rows, "tp")
            return jnp.concatenate(
                [jnp.where(tp == 0, rows, other), jnp.where(tp == 0, other, rows)], axis=0
            )

        def both_sequences(rows):
            away = swap(rows, "rep")
            return sequence(rows), sequence(away)

        def chip_sum(partial):
            other = swap(half(partial, 0, 1 - tp), "tp")
            return half(partial, 0, tp).astype(jnp.float32) + other.astype(jnp.float32)

        def project_out(mine, theirs, blocks, group):
            sums = []
            for start in range(0, len(blocks), group):
                weight = jnp.concatenate(blocks[start : start + group], axis=1)
                outs = []
                for rows in (theirs, mine):
                    outs.append(
                        jnp.dot(rows, weight, preferred_element_type=jnp.float32).astype(
                            jnp.bfloat16
                        )
                    )
                away = swap(chip_sum(outs[0]).astype(jnp.bfloat16), "rep")
                sums.append(chip_sum(outs[1]) + away.astype(jnp.float32))
            return jnp.concatenate(sums, axis=1)

        w_in = jnp.concatenate([half(w, 1, rep) for w in (w_bgate, w_cgate, w_value)], axis=1)
        w_gu = jnp.concatenate([half(w, 1, rep) for w in (w_gate, w_up)], axis=1)
        in_blocks = ring_first(w_in)
        out_blocks = ring_first(half(w_mixout, 0, rep))
        upper, lower = jnp.split(w_gu, 2, axis=0)
        gu_blocks = [part for both in zip(pair_first(upper), ring_first(lower)) for part in both]
        down_blocks = ring_first(half(w_down, 0, rep))

        channels = w_in.shape[1] // 3
        taps = lax.dynamic_slice_in_dim(conv_taps, (tp * 2 + rep) * channels, channels, 1)
        local = arrival_order(tokens)

        def mix(normed, weight):
            projected = jnp.dot(normed, weight, preferred_element_type=jnp.float32).astype(
                jnp.bfloat16
            )
            b_proj, c_proj, u_proj = (
                projected[:, k * channels : (k + 1) * channels].astype(jnp.float32)
                for k in range(3)
            )
            return (b_proj * causal_taps(c_proj * u_proj, taps)).astype(jnp.bfloat16)

        mine, theirs = both_sequences(
            rms_scale(local, arrival_order(mix_gain)).astype(jnp.bfloat16)
        )
        weight = jnp.concatenate(in_blocks, axis=0)
        theirs, mine = mix(theirs, weight), mix(mine, weight)
        mixed = project_out(mine, theirs, out_blocks, 2)
        residual = local.astype(jnp.float32) + mixed

        units = w_gu.shape[1] // 2

        def feed(normed, weight):
            both = jnp.dot(normed, weight, preferred_element_type=jnp.float32)
            return (jax.nn.silu(both[:, :units]) * both[:, units:]).astype(jnp.bfloat16)

        mine, theirs = both_sequences(
            rms_scale(residual, arrival_order(mlp_gain)).astype(jnp.bfloat16)
        )
        weight = jnp.concatenate(gu_blocks, axis=0)
        theirs, mine = feed(theirs, weight), feed(mine, weight)
        down = project_out(mine, theirs, down_blocks, 2)
        return global_order((residual + 0.5 * down).astype(jnp.bfloat16))

    return on_device


def solution(mesh):
    return jax.shard_map(
        build(mesh.shape["fs"]),
        mesh=mesh,
        in_specs=(
            P(("rep", "fs", "tp"), None),
            P(),
            P("fs", "tp"),
            P("fs", "tp"),
            P("fs", "tp"),
            P(),
            P("tp", "fs"),
            P(),
            P("fs", "tp"),
            P("fs", "tp"),
            P("tp", "fs"),
        ),
        out_specs=P(("rep", "fs", "tp"), None),
        check_vma=False,
    )
```
